32 devices in a mesh: ep: 8 (over z, x), tp: 4 (over y, core).
Axes of the slice: x: 2, y: 2, z: 4, core: 2. Of those that a mesh axis runs over, the one named last changes fastest.
Arguments:
- mixer_input: bfloat16 [1024, 2048], P('ep'), may hold values from -6 to 6
- mixer_gain: float32 [2048], replicated, may hold values from 0.1 to 1.9
- outer_weight: bfloat16 [2048, 1024], P(None, 'tp'), may hold values from -0.125 to 0.125
- inner_weight: bfloat16 [2048, 1024], P(None, 'tp'), may hold values from -0.125 to 0.125
- value_weight: bfloat16 [2048, 1024], P(None, 'tp'), may hold values from -0.125 to 0.125
- conv_kernel: bfloat16 [3, 1024], P(None, 'tp'), may hold values from -3 to 3
- group_gain: float32 [1024], P('tp'), may hold values from 0.1 to 1.9
- mixer_out_weight: bfloat16 [1024, 2048], P(None, 'tp'), may hold values from -0.1875 to 0.1875
- expert_input: bfloat16 [2048, 2048], P('ep'), may hold values from -6 to 6
- expert_gain: float32 [2048], replicated, may hold values from 0.1 to 1.9
- routes: int32 [2048, 2], P('ep'), may hold values from 0 to 7, all different within a row; in each aligned block of 256 rows (0 to 255, 256 to 511, ...) at most 128 rows name the same one
- route_weight: float32 [2048, 2], P('ep'), may hold values from 0.1 to 1
- expert_gate: bfloat16 [8, 2048, 3584], P('ep', None, 'tp'), may hold values from -0.125 to 0.125
- expert_up: bfloat16 [8, 2048, 3584], P('ep', None, 'tp'), may hold values from -0.125 to 0.125
- expert_down: bfloat16 [8, 3584, 2048], P('ep', None, 'tp'), may hold values from -0.09375 to 0.09375
Outputs:
- mixed_tokens: bfloat16 [1024, 2048], P('ep', 'tp')
- expert_tokens: bfloat16 [2048, 2048], P('ep', 'tp')
The draws below stay inside these ranges and needn't reach their ends.
Inputs may be any that keep to these rules, and one draw needn't show every extreme that they name: `routes`: each row names 2 different experts. Within the rows of one index of ep no expert is named by more than 128 rows, a bound that some block reaches of them.
All inputs are finite; a program needn't handle non-finite values.
Results may differ from the reference program's by a relative error of at most 0.014.
Values may be sent and summed in bfloat16 or wider, within the bound.
A program may use at most 64 MiB of HBM per device.

```python
import math
import jax
import jax.numpy as jnp
import numpy as np
from jax import lax

D = 2048
CONV = 1024
GROUP = 64
FF = 3584
TOP = 2
EXP_ROWS = 256
EXPERTS = 8
CAP = 128
MIX_TOKENS = 1024
EXP_TOKENS = 2048
N_EP = 8


def level_of(rng, extent, cuts, smallest, high):
    loudness = 1.0
    for dim, blocks in cuts:
        draws = jax.random.uniform(jax.random.fold_in(jax.random.fold_in(rng, 6), dim), (blocks,), jnp.float32, smallest / len(cuts), high / len(cuts))
        loudness = loudness * jnp.repeat(jnp.exp(draws), extent[dim] // blocks).reshape((-1,) + (1,) * (len(extent) - 1 - dim))
    return loudness


def assign_block(own_key, own, number, rows, count, top, bound, skew):
    ranking = jax.random.permutation(own_key, count)
    packed, common = load_shares(count, rows * top, bound, skew, True), load_shares(count, rows * top, bound, skew, False)
    places = jnp.arange(count)

    def named(tallies, turn):
        used = int((tallies > 0).sum())
        fixed = max(1, used // 4)
        passed = fixed + (places - fixed + turn * (used - fixed)) % max(1, count - fixed)
        return jnp.zeros((count,), jnp.int32).at[ranking[jnp.where(places < fixed, places, passed)]].set(jnp.asarray(tallies, jnp.int32))

    tallies = jnp.where(number % 4 == 0, named(packed, number // 4), named(common, number - number // 4 - 1))
    mixed = jax.random.permutation(jax.random.fold_in(own, 3), count)
    source_of, taker = mixed[0:count // 2 * 2:2], mixed[1:count // 2 * 2:2]
    room = jnp.minimum(tallies[source_of] - 1, bound - tallies[taker]) // 2
    room = jnp.where((source_of == ranking[0]) | (taker == ranking[0]) | (tallies[taker] == 0), 0, jnp.maximum(room, 0))
    passed = jax.random.randint(jax.random.fold_in(own, 4), (count // 2,), 0, 1 << 20) % (room + 1)
    tallies = tallies.at[source_of].add(-passed).at[taker].add(passed)
    members = jnp.searchsorted(jnp.cumsum(tallies), jnp.arange(rows * top), side="right").astype(jnp.int32)
    table = members.reshape(top, rows).T
    table = table[jax.random.permutation(jax.random.fold_in(own, 1), rows)]
    turn = jax.random.randint(jax.random.fold_in(own, 2), (rows, 1), 0, top)
    return jnp.take_along_axis(table, (jnp.arange(top)[None, :] + turn) % top, axis=1)


def load_shares(count, total, most, skew, full):
    loads = [(1 << 20) // math.isqrt(rank ** skew) + 1 for rank in range(1, count + 1)]
    largest = most if full else min(most, max(-(-total // count), total * loads[0] // sum(loads)))
    least = 1 if total - largest >= count - 1 else 0
    holding, surplus = [largest] + [least] * (count - 1), total - largest - least * (count - 1)
    while surplus > 0:
        movable = [i for i in range(1, count) if holding[i] < largest] or [i for i in range(1, count) if holding[i] < most]
        whole, remaining = sum([loads[i] for i in movable]), surplus
        for i in movable:
            addition = min(most - holding[i], max(1, remaining * loads[i] // whole), surplus)
            holding[i] = holding[i] + addition
            surplus = surplus - addition
    return np.array(holding)


def scatter_about(stream_key, dims, spread, limit, shards=(), kind=jnp.bfloat16):
    values = spread * jax.random.normal(stream_key, dims, jnp.float32)
    if shards:
        values = values * level_of(stream_key, dims, shards, -0.22, 0.18)
    return jnp.clip(values, -limit, limit).astype(kind)


def setup_inputs(seed: int = 0) -> dict:
    splits = jax.random.split(jax.random.key(seed), 16)
    mixer_input = scatter_about(splits[0], (MIX_TOKENS, D), 1.0, 6.0, ((0, 8),))
    mixer_gain = jnp.clip(1.0 + 0.18 * jax.random.normal(splits[1], (D,), jnp.float32), 0.1, 1.9)
    outer_weight = scatter_about(splits[2], (D, CONV), D ** -0.5, 0.125, ((1, 4),))
    inner_weight = scatter_about(splits[3], (D, CONV), D ** -0.5, 0.125, ((1, 4),))
    value_weight = scatter_about(splits[4], (D, CONV), D ** -0.5, 0.125, ((1, 4),))
    conv_kernel = scatter_about(splits[5], (3, CONV), 0.6, 3.0, ((1, 4),))
    group_gain = jnp.clip(1.0 + 0.18 * jax.random.normal(splits[6], (CONV,), jnp.float32), 0.1, 1.9)
    mixer_out_weight = scatter_about(splits[7], (CONV, D), CONV ** -0.5, 0.1875, ((1, 4),))
    expert_input = scatter_about(splits[8], (EXP_TOKENS, D), 1.0, 6.0, ((0, 8),))
    expert_gain = jnp.clip(1.0 + 0.18 * jax.random.normal(splits[9], (D,), jnp.float32), 0.1, 1.9)
    routes_keys = jax.random.split(jax.random.fold_in(splits[10], 1), EXP_TOKENS // EXP_ROWS)
    routes_turns = jax.random.permutation(jax.random.fold_in(splits[10], 3), EXP_TOKENS // EXP_ROWS)
    routes = jax.vmap(lambda own, number: assign_block(jax.random.fold_in(splits[10], 2), own, number, EXP_ROWS, EXPERTS, TOP, CAP, 2))(routes_keys, routes_turns).reshape((EXP_TOKENS, TOP))
    route_weight = jnp.clip(0.1 + 0.9 * jax.random.uniform(splits[11], (EXP_TOKENS, TOP), jnp.float32) ** level_of(splits[11], (EXP_TOKENS, TOP), ((0, 8),), -0.2, 0.2), 0.1, 1.0)
    expert_gate = scatter_about(splits[12], (EXPERTS, D, FF), D ** -0.5, 0.125, ((0, 8), (2, 4)))
    expert_up = scatter_about(splits[13], (EXPERTS, D, FF), D ** -0.5, 0.125, ((0, 8), (2, 4)))
    expert_down = scatter_about(splits[14], (EXPERTS, FF, D), FF ** -0.5, 0.09375, ((0, 8), (2, 4)))
    return dict(mixer_input=mixer_input, mixer_gain=mixer_gain, outer_weight=outer_weight, inner_weight=inner_weight, value_weight=value_weight, conv_kernel=conv_kernel, group_gain=group_gain, mixer_out_weight=mixer_out_weight, expert_input=expert_input, expert_gain=expert_gain, routes=routes, route_weight=route_weight, expert_gate=expert_gate, expert_up=expert_up, expert_down=expert_down)


EPS = 1e-06

def rms_scale(values, gain):
    floats = values.astype(jnp.float32)
    scale = lax.rsqrt(lax.optimization_barrier(jnp.mean(floats * floats, axis=-1, keepdims=True)) + EPS)
    return floats * scale * gain.astype(jnp.float32)

def run_expert(operands):
    rows, gate_part, up_part, down_part = operands
    gate = jnp.dot(rows, gate_part, preferred_element_type=jnp.float32)
    up_value = jnp.dot(rows, up_part, preferred_element_type=jnp.float32)
    hidden = (jax.nn.silu(gate) * up_value).astype(jnp.bfloat16)
    return jnp.dot(hidden, down_part, preferred_element_type=jnp.float32).astype(jnp.bfloat16)

def reference(mixer_input, mixer_gain, outer_weight, inner_weight, value_weight, conv_kernel, group_gain, mixer_out_weight, expert_input, expert_gain, routes, route_weight, expert_gate, expert_up, expert_down):
    count = mixer_input.shape[0]
    normed_a = rms_scale(mixer_input, mixer_gain).astype(jnp.bfloat16)
    outer = jnp.dot(normed_a, outer_weight, preferred_element_type=jnp.float32).astype(jnp.bfloat16)
    inner = jnp.dot(normed_a, inner_weight, preferred_element_type=jnp.float32).astype(jnp.bfloat16)
    values = jnp.dot(normed_a, value_weight, preferred_element_type=jnp.float32).astype(jnp.bfloat16)
    product = inner.astype(jnp.float32) * values.astype(jnp.float32)
    padded = jnp.pad(product, ((2, 0), (0, 0)))
    kernel = conv_kernel.astype(jnp.float32)
    conv_sum = kernel[0] * padded[0:count] + kernel[1] * padded[1:count + 1] + kernel[2] * padded[2:count + 2]
    gated = outer.astype(jnp.float32) * conv_sum
    grouped = gated.reshape(count, CONV // GROUP, GROUP)
    grouped = rms_scale(grouped, group_gain.reshape(CONV // GROUP, GROUP))
    grouped = grouped.reshape(count, CONV).astype(jnp.bfloat16)
    mixed_tokens = jnp.dot(grouped, mixer_out_weight, preferred_element_type=jnp.float32).astype(jnp.bfloat16)
    normed_b = rms_scale(expert_input, expert_gain).astype(jnp.bfloat16)
    picks = routes.reshape(N_EP, EXP_ROWS * TOP).astype(jnp.int32)
    onehot = (picks[:, :, None] == jnp.arange(EXPERTS, dtype=jnp.int32)[None, None, :]).astype(jnp.int32)
    earlier = jnp.cumsum(onehot, axis=1) - onehot
    rank = lax.optimization_barrier(jnp.sum(earlier * onehot, axis=2)).astype(jnp.int32)
    slot = (picks * CAP + rank).astype(jnp.int32)
    token = (jnp.arange(EXP_ROWS * TOP, dtype=jnp.int32) // TOP).astype(jnp.int32)
    source = jnp.arange(N_EP, dtype=jnp.int32)[:, None]
    table = jnp.zeros((N_EP, EXPERTS * CAP), jnp.int32).at[source, slot].set(token[None, :] + 1)
    valid = table > 0
    row_index = (source * EXP_ROWS + jnp.maximum(table - 1, 0)).astype(jnp.int32)
    buffer = jnp.where(valid[..., None], jnp.take(normed_b, row_index, axis=0), 0).astype(jnp.bfloat16)
    per_expert = buffer.reshape(N_EP, EXPERTS, CAP, D).transpose(1, 0, 2, 3).reshape(EXPERTS, N_EP * CAP, D)
    outputs = lax.map(run_expert, (per_expert, expert_gate, expert_up, expert_down))
    flat_out = outputs.reshape(EXPERTS * N_EP * CAP, D)
    position = (picks * (N_EP * CAP) + source * CAP + rank).astype(jnp.int32)
    chosen = jnp.take(flat_out, position.reshape(-1), axis=0).astype(jnp.float32).reshape(N_EP * EXP_ROWS, TOP, D)
    weighted = lax.optimization_barrier(jnp.sum(chosen * route_weight.astype(jnp.float32)[..., None], axis=1))
    expert_tokens = weighted.astype(jnp.bfloat16)
    return (mixed_tokens, expert_tokens)
```

```python
import functools

import jax
import jax.numpy as jnp
from jax import lax
from jax.experimental import pallas as pl
from jax.experimental.pallas import tpu as pltpu
from jax.sharding import PartitionSpec as P

GROUP = 64


EPS = 1e-06


def from_behind(block, axis, distance):
    devices = range(lax.axis_size(axis))
    route = [(i - distance, i) for i in devices if i - distance in devices]
    return lax.ppermute(block, axis, route)


def rms_scale(values, gain):
    floats = values.astype(jnp.float32)
    scale = lax.rsqrt(jnp.mean(floats * floats, axis=-1, keepdims=True) + EPS)
    return floats * scale * gain


F32 = jnp.float32
BF16 = jnp.bfloat16


def flip(index, offset, count):
    out = index
    bit = 1
    while bit < count:
        if offset & bit:
            out = out + bit - 2 * bit * ((index // bit) % 2)
        bit *= 2
    return out


def matmul(a, b):
    return jnp.dot(a, b, preferred_element_type=F32)


def experts_kernel(
    n_ep,
    x_ref,
    gain_ref,
    routes_ref,
    weight_ref,
    gate_hbm,
    up_hbm,
    down_hbm,
    o_ref,
    nb,
    xs,
    xb,
    wgu,
    wd,
    hb,
    rs,
    ret,
    whi,
    wlo,
    w_sem,
    s_sem,
    r_sem,
):
    ep = lax.axis_index("ep")
    tp = lax.axis_index("tp")
    y, core = tp // 2, tp % 2
    partner = {"tp": y * 2 + 1 - core}
    across = {"tp": (1 - y) * 2 + core}
    over_tp = (1 - y) * 2 + core
    half = n_ep // 2
    rows = x_ref.shape[0]
    cap = xb.shape[2]
    span = xb.shape[3]
    tiles, depth, pair = wgu.shape
    tile = pair // 2
    part = hb.shape[3]
    out_cols = wd.shape[1]

    barrier = pltpu.get_barrier_semaphore()
    peers = [{"ep": flip(ep, m, n_ep)} for m in range(1, n_ep)] + [partner, across]
    for peer in peers:
        pl.semaphore_signal(barrier, inc=1, device_id=peer, device_id_type=pl.DeviceIdType.MESH)

    fetches = []
    for j in range(tiles):
        cols = pl.ds(j * tile, tile)
        fetches.append(
            (
                pltpu.make_async_copy(
                    gate_hbm.at[0, :, cols], wgu.at[j, :, pl.ds(0, tile)], w_sem.at[2 * j]
                ),
                pltpu.make_async_copy(
                    up_hbm.at[0, :, cols], wgu.at[j, :, pl.ds(tile, tile)], w_sem.at[2 * j + 1]
                ),
            )
        )
    fetch_down = pltpu.make_async_copy(down_hbm.at[0], wd, w_sem.at[2 * tiles])
    for a, b in fetches:
        a.start()
        b.start()
    fetch_down.start()

    step_rows = 32

    def norm(i, carry):
        at = pl.ds(pl.multiple_of(i * step_rows, step_rows), step_rows)
        v = x_ref[at, :].astype(F32)
        scale = lax.rsqrt(jnp.mean(v * v, axis=-1, keepdims=True) + EPS)
        nb[at, :] = (v * scale * gain_ref[...]).astype(BF16)
        return carry

    lax.fori_loop(0, rows // step_rows, norm, 0)

    first = routes_ref[0:1, :]
    second = routes_ref[1:2, :]
    masks = []
    level = lax.broadcasted_iota(jnp.int32, (n_ep, rows), 0)
    stacked = jnp.zeros((n_ep, rows), F32)
    for m in range(n_ep):
        e = flip(ep, m, n_ep)
        mask = jnp.where((first == e) | (second == e), 1.0, 0.0)
        masks.append(mask)
        stacked = jnp.where(level == m, mask, stacked)
    upper = lax.broadcasted_iota(jnp.int32, (rows, rows), 0) < lax.broadcasted_iota(
        jnp.int32, (rows, rows), 1
    )
    ranks = matmul(stacked.astype(BF16), jnp.where(upper, 1.0, 0.0).astype(BF16))
    slots = lax.broadcasted_iota(jnp.int32, (cap, rows), 0).astype(F32)
    place = []
    for m in range(n_ep):
        place.append(jnp.where((slots == ranks[m : m + 1, :]) & (masks[m] > 0.5), 1.0, 0.0))

    def remote(src, dst, kind, m, device):
        return pltpu.make_async_remote_copy(
            src_ref=src,
            dst_ref=dst,
            send_sem=s_sem.at[kind, m],
            recv_sem=r_sem.at[kind, m],
            device_id=device,
            device_id_type=pl.DeviceIdType.MESH,
        )

    mine2 = pl.ds(core * 2, 2)
    from_source, to_partner, to_across, relay = [None] * n_ep, {}, {}, {}
    for m in range(1, n_ep):
        peer = {"ep": flip(ep, m, n_ep)}
        if m < half:
            from_source[m] = remote(xs.at[m], xb.at[m, mine2], 0, m, peer)
            to_partner[m] = remote(xb.at[m, mine2], xb.at[m, mine2], 1, m, partner)
        else:
            from_source[m] = remote(xs.at[m, 0], xb.at[m, tp], 0, m, peer)
            to_partner[m] = remote(xb.at[m, tp], xb.at[m, tp], 1, m, partner)
            to_across[m] = remote(xb.at[m, tp], xb.at[m, tp], 2, m, across)
            relay[m] = remote(xb.at[m, over_tp], xb.at[m, over_tp], 3, m, partner)
    hid_partner, hid_across, hid_relay, back = [], [], [], [None] * n_ep
    for m in range(n_ep):
        hid_partner.append(remote(hb.at[m, tp], hb.at[m, tp], 4, m, partner))
        hid_across.append(remote(hb.at[m, tp], hb.at[m, tp], 5, m, across))
        hid_relay.append(remote(hb.at[m, over_tp], hb.at[m, over_tp], 6, m, partner))
        if m:
            back[m] = remote(rs.at[m], ret.at[m], 7, m, {"ep": flip(ep, m, n_ep)})

    for m in range(1, n_ep):
        chosen = place[m].astype(BF16)
        if m < half:
            for k in range(2):
                at = pl.ds(pl.multiple_of((core * 2 + k) * span, span), span)
                xs[m, k] = matmul(chosen, nb[:, at]).astype(BF16)
        else:
            at = pl.ds(pl.multiple_of(tp * span, span), span)
            xs[m, 0] = matmul(chosen, nb[:, at]).astype(BF16)
        if m == 1:
            pl.semaphore_wait(barrier, len(peers))
        from_source[m].start()
    chosen = place[0].astype(BF16)
    for k in range(depth // span):
        xb[0, k] = matmul(chosen, nb[:, k * span : (k + 1) * span]).astype(BF16)

    def expand(m):
        def body(j, carry):
            if m == 0:
                pltpu.make_async_copy(
                    gate_hbm.at[0, :, pl.ds(0, tile)], wgu.at[j, :, pl.ds(0, tile)], w_sem.at[2 * j]
                ).wait()
                pltpu.make_async_copy(
                    up_hbm.at[0, :, pl.ds(0, tile)],
                    wgu.at[j, :, pl.ds(tile, tile)],
                    w_sem.at[2 * j + 1],
                ).wait()
            acc = matmul(xb[m, 0], wgu[j, 0:span, :])
            for k in range(1, depth // span):
                acc = acc + matmul(xb[m, k], wgu[j, k * span : (k + 1) * span, :])
            g, u = acc[:, :tile], acc[:, tile:]
            hidden = g / (1.0 + jnp.exp(-g)) * u
            hb[m, tp, :, pl.ds(pl.multiple_of(j * tile, tile), tile)] = hidden.astype(BF16)
            return carry

        lax.fori_loop(0, tiles, body, 0)
        hid_across[m].start()
        hid_partner[m].start()

    block = 256

    def contract(m):
        hid_partner[m].wait_recv()
        hid_relay[m].wait_recv()
        for n in range(out_cols // block):
            cols = slice(n * block, (n + 1) * block)
            acc = matmul(hb[m, 0], wd[0:part, cols])
            for k in range(1, hb.shape[1]):
                acc = acc + matmul(hb[m, k], wd[k * part : (k + 1) * part, cols])
            if m == 0:
                ret[0, :, cols] = acc.astype(BF16)
            else:
                rs[m, :, cols] = acc.astype(BF16)
        if m:
            back[m].start()

    def pass_hidden(m):
        hid_across[m].wait_recv()
        hid_relay[m].start()

    def pass_near(m):
        from_source[m].wait_recv()
        to_partner[m].start()

    def pass_far(m):
        from_source[m].wait_recv()
        to_across[m].start()
        to_partner[m].start()

    def pass_relay(m):
        to_across[m].wait_recv()
        relay[m].start()

    def ready(m):
        to_partner[m].wait_recv()
        if m >= half:
            relay[m].wait_recv()

    expand(0)
    for m in range(n_ep):
        picked = jnp.where(first == flip(ep, m, n_ep), weight_ref[0:1, :], weight_ref[1:2, :])
        scaled = (place[m] * picked).T
        high = scaled.astype(BF16)
        whi[:, m * cap : (m + 1) * cap] = high
        wlo[:, m * cap : (m + 1) * cap] = (scaled - high.astype(F32)).astype(BF16)
    for m in range(1, half):
        pass_near(m)
        ready(m)
        expand(m)
        if m == 1:
            fetch_down.wait()
        if m >= 2:
            pass_hidden(m - 2)
            contract(m - 2)
    for m in range(half, n_ep):
        pass_far(m)
        if m == half:
            pass_hidden(half - 2)
            contract(half - 2)
    pass_hidden(half - 1)
    for m in range(half, n_ep):
        pass_relay(m)
        ready(m)
        expand(m)
        if m == half:
            contract(half - 1)
        if m - 2 >= half:
            pass_hidden(m - 2)
            contract(m - 2)
    pass_hidden(n_ep - 2)
    contract(n_ep - 2)
    pass_hidden(n_ep - 1)
    contract(n_ep - 1)

    total = None
    for m in range(n_ep):
        if m:
            back[m].wait_recv()
        high = matmul(whi[:, m * cap : (m + 1) * cap], ret[m])
        low = matmul(wlo[:, m * cap : (m + 1) * cap], ret[m])
        total = high + low if total is None else total + (high + low)
    o_ref[...] = total.astype(BF16)

    for m in range(n_ep):
        for copy in (hid_partner[m], hid_across[m], hid_relay[m], from_source[m], back[m]):
            if copy is not None:
                copy.wait_send()
        for table in (to_partner, to_across, relay):
            if m in table:
                table[m].wait_send()


def experts_fused(
    expert_input, expert_gain, routes, route_weight, expert_gate, expert_up, expert_down
):
    n_ep, n_tp = lax.axis_size("ep"), lax.axis_size("tp")
    rows, width = expert_input.shape
    cap = 2 * routes.shape[1] * rows // n_ep
    span = width // n_tp
    part = expert_gate.shape[2]
    tile = 128
    tiles = part // tile
    full, out_cols = expert_down.shape[1:]
    vmem = pl.BlockSpec(memory_space=pltpu.VMEM)
    hbm = pl.BlockSpec(memory_space=pl.ANY)
    return pl.pallas_call(
        functools.partial(experts_kernel, n_ep),
        out_shape=jax.ShapeDtypeStruct((rows, out_cols), BF16),
        in_specs=[vmem] * 4 + [hbm] * 3,
        out_specs=vmem,
        scratch_shapes=[
            pltpu.VMEM((rows, width), BF16),
            pltpu.VMEM((n_ep, 2, cap, span), BF16),
            pltpu.VMEM((n_ep, n_tp, cap, span), BF16),
            pltpu.VMEM((tiles, width, 2 * tile), BF16),
            pltpu.VMEM((full, out_cols), BF16),
            pltpu.VMEM((n_ep, n_tp, cap, part), BF16),
            pltpu.VMEM((n_ep, cap, out_cols), BF16),
            pltpu.VMEM((n_ep, cap, out_cols), BF16),
            pltpu.VMEM((rows, n_ep * cap), BF16),
            pltpu.VMEM((rows, n_ep * cap), BF16),
            pltpu.SemaphoreType.DMA((2 * tiles + 1,)),
            pltpu.SemaphoreType.DMA((8, n_ep)),
            pltpu.SemaphoreType.DMA((8, n_ep)),
        ],
        compiler_params=pltpu.CompilerParams(
            collective_id=0, has_side_effects=True, vmem_limit_bytes=56 * 1024 * 1024
        ),
        name="experts",
    )(
        expert_input,
        expert_gain.reshape(1, -1),
        routes.T,
        route_weight.T,
        expert_gate,
        expert_up,
        expert_down,
    )


def fits(n_ep, n_tp, routes, expert_gate):
    return (
        n_tp == 4
        and n_ep >= 4
        and n_ep & (n_ep - 1) == 0
        and routes.shape[1] == 2
        and expert_gate.shape[0] == 1
        and expert_gate.shape[2] % 128 == 0
    )


def mixer_xla(
    mixer_input,
    mixer_gain,
    outer_weight,
    inner_weight,
    value_weight,
    conv_kernel,
    group_gain,
    mixer_out_weight,
):
    mix_count = mixer_input.shape[0]
    normed_a = rms_scale(mixer_input, mixer_gain).astype(jnp.bfloat16)
    outer = jnp.dot(normed_a, outer_weight, preferred_element_type=jnp.float32).astype(jnp.bfloat16)
    inner = jnp.dot(normed_a, inner_weight, preferred_element_type=jnp.float32).astype(jnp.bfloat16)
    values = jnp.dot(normed_a, value_weight, preferred_element_type=jnp.float32).astype(
        jnp.bfloat16
    )
    product = inner.astype(jnp.float32) * values.astype(jnp.float32)
    earlier_rows = from_behind(product[mix_count - 2 :], "ep", 1)
    padded = jnp.concatenate([earlier_rows, product], axis=0)
    kernel = conv_kernel.astype(jnp.float32)
    conv_sum = (
        kernel[0] * padded[0:mix_count]
        + kernel[1] * padded[1 : mix_count + 1]
        + kernel[2] * padded[2 : mix_count + 2]
    )
    gated = outer.astype(jnp.float32) * conv_sum
    grouped = gated.reshape(mix_count, -1, GROUP)
    grouped = rms_scale(grouped, group_gain.reshape(-1, GROUP))
    grouped = grouped.reshape(mix_count, -1).astype(jnp.bfloat16)
    weight_rows = mixer_out_weight
    mixed_tokens = jnp.dot(
        lax.all_gather(grouped, "tp", axis=1, tiled=True),
        weight_rows,
        preferred_element_type=jnp.float32,
    ).astype(jnp.bfloat16)
    return mixed_tokens


def experts_xla(
    expert_input,
    expert_gain,
    routes,
    route_weight,
    expert_gate,
    expert_up,
    expert_down,
):
    exp_count, picks_each = routes.shape
    width = expert_input.shape[1]
    experts = expert_gate.shape[0] * lax.axis_size("ep")
    capacity = 2 * picks_each * exp_count // experts
    normed_b = rms_scale(expert_input, expert_gain).astype(jnp.bfloat16)
    picks = routes.reshape(-1)
    onehot = (picks[:, None] == jnp.arange(experts, dtype=jnp.int32)[None, :]).astype(jnp.int32)
    rank = jnp.sum((jnp.cumsum(onehot, axis=0) - onehot) * onehot, axis=1)
    slot = picks * capacity + rank
    token = jnp.arange(exp_count * picks_each, dtype=jnp.int32) // picks_each
    table = jnp.zeros((experts * capacity,), jnp.int32).at[slot].set(token + 1)
    valid = table > 0
    gathered_rows = jnp.take(normed_b, jnp.maximum(table - 1, 0), axis=0)
    buffer = jnp.where(valid[:, None], gathered_rows, 0).reshape(experts, capacity, width)
    gate_weight = expert_gate[0]
    up_weight = expert_up[0]
    down_weight = expert_down[0]
    out_cols = down_weight.shape[1]
    span = width // lax.axis_size("tp")
    outgoing = lax.dynamic_slice_in_dim(buffer, lax.axis_index("tp") * span, span, 2)
    received = lax.all_to_all(outgoing, "ep", split_axis=0, concat_axis=0, tiled=True)
    sources = received.shape[0]
    count = received.shape[1]
    piece = lax.all_gather(received, "tp", axis=2, tiled=True)
    span = piece.shape[2]
    flat_piece = piece.reshape(sources * count, span)
    gate = jnp.dot(flat_piece, gate_weight, preferred_element_type=jnp.float32)
    up_value = jnp.dot(flat_piece, up_weight, preferred_element_type=jnp.float32)
    hidden = (jax.nn.silu(gate) * up_value).astype(jnp.bfloat16)
    weight_rows = down_weight
    results = jnp.dot(
        lax.all_gather(hidden, "tp", axis=1, tiled=True),
        weight_rows,
        preferred_element_type=jnp.float32,
    ).astype(jnp.bfloat16)
    returned = lax.all_to_all(
        results.reshape(sources, count, out_cols), "ep", split_axis=0, concat_axis=0, tiled=True
    )
    flat_returned = returned.reshape(experts * capacity, out_cols)
    chosen = (
        jnp.take(flat_returned, slot, axis=0)
        .astype(jnp.float32)
        .reshape(exp_count, picks_each, out_cols)
    )
    weighted = jnp.sum(chosen * route_weight[..., None], axis=1)
    expert_tokens = weighted.astype(jnp.bfloat16)
    return expert_tokens


def per_device(*args):
    mixed = mixer_xla(*args[:8])
    n_ep, n_tp = lax.axis_size("ep"), lax.axis_size("tp")
    if fits(n_ep, n_tp, args[10], args[12]):
        return mixed, experts_fused(*args[8:])
    return mixed, experts_xla(*args[8:])


def solution(mesh):
    placed = (
        P("ep", None),
        P(),
        P(None, "tp"),
        P(None, "tp"),
        P(None, "tp"),
        P(None, "tp"),
        P("tp"),
        P(None, "tp"),
        P("ep", None),
        P(),
        P("ep", None),
        P("ep", None),
        P("ep", None, "tp"),
        P("ep", None, "tp"),
        P("ep", None, "tp"),
    )
    return jax.shard_map(
        per_device,
        mesh=mesh,
        in_specs=placed,
        out_specs=(P("ep", "tp"), P("ep", "tp")),
        check_vma=False,
    )
```

```python
import functools

import jax
import jax.numpy as jnp
from jax import lax
from jax.experimental import pallas as pl
from jax.experimental.pallas import tpu as pltpu
from jax.sharding import PartitionSpec as P

GROUP = 64


EPS = 1e-06


def from_behind(block, axis, distance):
    devices = range(lax.axis_size(axis))
    route = [(i - distance, i) for i in devices if i - distance in devices]
    return lax.ppermute(block, axis, route)


def rms_scale(values, gain):
    floats = values.astype(jnp.float32)
    scale = lax.rsqrt(jnp.mean(floats * floats, axis=-1, keepdims=True) + EPS)
    return floats * scale * gain


F32 = jnp.float32
BF16 = jnp.bfloat16


def flip(index, offset, count):
    out = index
    bit = 1
    while bit < count:
        if offset & bit:
            out = out + bit - 2 * bit * ((index // bit) % 2)
        bit *= 2
    return out


def matmul(a, b):
    return jnp.dot(a, b, preferred_element_type=F32)


def experts_kernel(
    n_ep,
    mix_ref,
    mix_gain_ref,
    kernel_ref,
    group_gain_ref,
    x_ref,
    gain_ref,
    routes_ref,
    weight_ref,
    outer_hbm,
    inner_hbm,
    value_hbm,
    mix_out_hbm,
    gate_hbm,
    up_hbm,
    down_hbm,
    mix_o_ref,
    o_ref,
    nb,
    xs,
    xb,
    wgu,
    wd,
    hb,
    rs,
    ret,
    whi,
    wlo,
    na,
    wmix,
    wmo,
    padded,
    outer,
    grouped,
    w_sem,
    s_sem,
    r_sem,
):
    ep = lax.axis_index("ep")
    tp = lax.axis_index("tp")
    y, core = tp // 2, tp % 2
    partner = {"tp": y * 2 + 1 - core}
    across = {"tp": (1 - y) * 2 + core}
    over_tp = (1 - y) * 2 + core
    half = n_ep // 2
    rows = x_ref.shape[0]
    cap = xb.shape[2]
    span = xb.shape[3]
    tiles, depth, pair = wgu.shape
    tile = pair // 2
    part = hb.shape[3]
    out_cols = wd.shape[1]

    barrier = pltpu.get_barrier_semaphore()
    peers = [{"ep": flip(ep, m, n_ep)} for m in range(1, n_ep)] + [partner, across]
    for peer in peers:
        pl.semaphore_signal(barrier, inc=1, device_id=peer, device_id_type=pl.DeviceIdType.MESH)

    fetches = []
    for j in range(tiles):
        cols = pl.ds(j * tile, tile)
        fetches.append(
            (
                pltpu.make_async_copy(
                    gate_hbm.at[0, :, cols], wgu.at[j, :, pl.ds(0, tile)], w_sem.at[2 * j]
                ),
                pltpu.make_async_copy(
                    up_hbm.at[0, :, cols], wgu.at[j, :, pl.ds(tile, tile)], w_sem.at[2 * j + 1]
                ),
            )
        )
    fetch_down = pltpu.make_async_copy(down_hbm.at[0], wd, w_sem.at[2 * tiles])
    fetch_mix = [
        pltpu.make_async_copy(src, wmix.at[i], w_sem.at[2 * tiles + 1 + i])
        for i, src in enumerate((outer_hbm, inner_hbm, value_hbm))
    ]
    fetch_mix_out = pltpu.make_async_copy(mix_out_hbm, wmo, w_sem.at[2 * tiles + 4])
    for a, b in fetches:
        a.start()
        b.start()
    for copy in fetch_mix:
        copy.start()
    fetch_down.start()
    fetch_mix_out.start()

    step_rows = 32

    def normalize(src, gain, dst):
        def norm(i, carry):
            at = pl.ds(pl.multiple_of(i * step_rows, step_rows), step_rows)
            v = src[at, :].astype(F32)
            scale = lax.rsqrt(jnp.mean(v * v, axis=-1, keepdims=True) + EPS)
            dst[at, :] = (v * scale * gain[...]).astype(BF16)
            return carry

        lax.fori_loop(0, src.shape[0] // step_rows, norm, 0)

    normalize(x_ref, gain_ref, nb)

    first = routes_ref[0:1, :]
    second = routes_ref[1:2, :]
    masks = []
    level = lax.broadcasted_iota(jnp.int32, (n_ep, rows), 0)
    stacked = jnp.zeros((n_ep, rows), F32)
    for m in range(n_ep):
        e = flip(ep, m, n_ep)
        mask = jnp.where((first == e) | (second == e), 1.0, 0.0)
        masks.append(mask)
        stacked = jnp.where(level == m, mask, stacked)
    upper = lax.broadcasted_iota(jnp.int32, (rows, rows), 0) < lax.broadcasted_iota(
        jnp.int32, (rows, rows), 1
    )
    ranks = matmul(stacked.astype(BF16), jnp.where(upper, 1.0, 0.0).astype(BF16))
    slots = lax.broadcasted_iota(jnp.int32, (cap, rows), 0).astype(F32)
    place = []
    for m in range(n_ep):
        place.append(jnp.where((slots == ranks[m : m + 1, :]) & (masks[m] > 0.5), 1.0, 0.0))

    def remote(src, dst, kind, m, device):
        return pltpu.make_async_remote_copy(
            src_ref=src,
            dst_ref=dst,
            send_sem=s_sem.at[kind, m],
            recv_sem=r_sem.at[kind, m],
            device_id=device,
            device_id_type=pl.DeviceIdType.MESH,
        )

    mine2 = pl.ds(core * 2, 2)
    from_source, to_partner, to_across, relay = [None] * n_ep, {}, {}, {}
    for m in range(1, n_ep):
        peer = {"ep": flip(ep, m, n_ep)}
        if m < half:
            from_source[m] = remote(xs.at[m], xb.at[m, mine2], 0, m, peer)
            to_partner[m] = remote(xb.at[m, mine2], xb.at[m, mine2], 1, m, partner)
        else:
            from_source[m] = remote(xs.at[m, 0], xb.at[m, tp], 0, m, peer)
            to_partner[m] = remote(xb.at[m, tp], xb.at[m, tp], 1, m, partner)
            to_across[m] = remote(xb.at[m, tp], xb.at[m, tp], 2, m, across)
            relay[m] = remote(xb.at[m, over_tp], xb.at[m, over_tp], 3, m, partner)
    hid_partner, hid_across, hid_relay, back = [], [], [], [None] * n_ep
    for m in range(n_ep):
        hid_partner.append(remote(hb.at[m, tp], hb.at[m, tp], 4, m, partner))
        hid_across.append(remote(hb.at[m, tp], hb.at[m, tp], 5, m, across))
        hid_relay.append(remote(hb.at[m, over_tp], hb.at[m, over_tp], 6, m, partner))
        if m:
            back[m] = remote(rs.at[m], ret.at[m], 7, m, {"ep": flip(ep, m, n_ep)})

    for m in range(1, n_ep):
        chosen = place[m].astype(BF16)
        if m < half:
            for k in range(2):
                at = pl.ds(pl.multiple_of((core * 2 + k) * span, span), span)
                xs[m, k] = matmul(chosen, nb[:, at]).astype(BF16)
        else:
            at = pl.ds(pl.multiple_of(tp * span, span), span)
            xs[m, 0] = matmul(chosen, nb[:, at]).astype(BF16)
        if m == 1:
            pl.semaphore_wait(barrier, len(peers))
        from_source[m].start()
    chosen = place[0].astype(BF16)
    for k in range(depth // span):
        xb[0, k] = matmul(chosen, nb[:, k * span : (k + 1) * span]).astype(BF16)

    def expand(m):
        def body(j, carry):
            if m == 0:
                pltpu.make_async_copy(
                    gate_hbm.at[0, :, pl.ds(0, tile)], wgu.at[j, :, pl.ds(0, tile)], w_sem.at[2 * j]
                ).wait()
                pltpu.make_async_copy(
                    up_hbm.at[0, :, pl.ds(0, tile)],
                    wgu.at[j, :, pl.ds(tile, tile)],
                    w_sem.at[2 * j + 1],
                ).wait()
            acc = matmul(xb[m, 0], wgu[j, 0:span, :])
            for k in range(1, depth // span):
                acc = acc + matmul(xb[m, k], wgu[j, k * span : (k + 1) * span, :])
            g, u = acc[:, :tile], acc[:, tile:]
            hidden = g / (1.0 + jnp.exp(-g)) * u
            hb[m, tp, :, pl.ds(pl.multiple_of(j * tile, tile), tile)] = hidden.astype(BF16)
            return carry

        lax.fori_loop(0, tiles, body, 0)
        hid_across[m].start()
        hid_partner[m].start()

    block = 256

    def contract(m):
        hid_partner[m].wait_recv()
        hid_relay[m].wait_recv()
        for n in range(out_cols // block):
            cols = slice(n * block, (n + 1) * block)
            acc = matmul(hb[m, 0], wd[0:part, cols])
            for k in range(1, hb.shape[1]):
                acc = acc + matmul(hb[m, k], wd[k * part : (k + 1) * part, cols])
            if m == 0:
                ret[0, :, cols] = acc.astype(BF16)
            else:
                rs[m, :, cols] = acc.astype(BF16)
        if m:
            back[m].start()

    def pass_hidden(m):
        hid_across[m].wait_recv()
        hid_relay[m].start()

    def pass_near(m):
        from_source[m].wait_recv()
        to_partner[m].start()

    def pass_far(m):
        from_source[m].wait_recv()
        to_across[m].start()
        to_partner[m].start()

    def pass_relay(m):
        to_across[m].wait_recv()
        relay[m].start()

    def ready(m):
        to_partner[m].wait_recv()
        if m >= half:
            relay[m].wait_recv()

    mix_rows, channels = outer.shape
    halo = padded.shape[0] - mix_rows
    ahead = {"ep": lax.rem(ep + 1, n_ep)}
    send_halo = remote(padded.at[pl.ds(mix_rows, halo)], padded.at[pl.ds(0, halo)], 8, 0, ahead)
    mix_partner = remote(grouped.at[tp], grouped.at[tp], 8, 1, partner)
    mix_across = remote(grouped.at[tp], grouped.at[tp], 8, 2, across)
    mix_relay = remote(grouped.at[over_tp], grouped.at[over_tp], 8, 3, partner)

    def mix_project():
        normalize(mix_ref, mix_gain_ref, na)
        for copy in fetch_mix:
            copy.wait()
        outer[...] = matmul(na[...], wmix[0]).astype(BF16)
        inner = matmul(na[...], wmix[1]).astype(BF16).astype(F32)
        padded[pl.ds(halo, mix_rows), :] = inner * matmul(na[...], wmix[2]).astype(BF16).astype(F32)
        send_halo.start()

    def mix_convolve():
        send_halo.wait_recv()
        taps = kernel_ref[...].astype(F32)
        row = lax.broadcasted_iota(jnp.int32, (mix_rows, channels), 0)
        row = row + jnp.where(ep == 0, 0, mix_rows)
        conv = taps[2:3, :] * padded[pl.ds(halo, mix_rows), :]
        for back_by in (1, 2):
            shifted = padded[pl.ds(halo - back_by, mix_rows), :]
            conv = conv + taps[2 - back_by : 3 - back_by, :] * jnp.where(
                row >= back_by, shifted, 0.0
            )
        gated = outer[...].astype(F32) * conv
        squares = gated * gated
        group = lax.broadcasted_iota(jnp.int32, (mix_rows, channels), 1) // GROUP
        scale = jnp.zeros_like(gated)
        for i in range(channels // GROUP):
            mean = jnp.sum(jnp.where(group == i, squares, 0.0), axis=-1, keepdims=True) / GROUP
            scale = jnp.where(group == i, lax.rsqrt(mean + EPS), scale)
        grouped[tp] = (gated * scale * group_gain_ref[...]).astype(BF16)
        mix_across.start()
        mix_partner.start()

    def mix_pass():
        mix_across.wait_recv()
        mix_relay.start()

    def mix_contract():
        fetch_mix_out.wait()
        mix_partner.wait_recv()
        mix_relay.wait_recv()
        acc = matmul(grouped[0], wmo[0:channels, :])
        for k in range(1, grouped.shape[0]):
            acc = acc + matmul(grouped[k], wmo[k * channels : (k + 1) * channels, :])
        mix_o_ref[...] = acc.astype(BF16)

    expand(0)
    mix_project()
    for m in range(n_ep):
        picked = jnp.where(first == flip(ep, m, n_ep), weight_ref[0:1, :], weight_ref[1:2, :])
        scaled = (place[m] * picked).T
        high = scaled.astype(BF16)
        whi[:, m * cap : (m + 1) * cap] = high
        wlo[:, m * cap : (m + 1) * cap] = (scaled - high.astype(F32)).astype(BF16)
    for m in range(1, half):
        pass_near(m)
        ready(m)
        expand(m)
        if m == 1:
            mix_convolve()
            fetch_down.wait()
        if m >= 2:
            pass_hidden(m - 2)
            contract(m - 2)
    for m in range(half, n_ep):
        pass_far(m)
        if m == half:
            pass_hidden(half - 2)
            contract(half - 2)
        if m == half:
            mix_pass()
    pass_hidden(half - 1)
    mix_contract()
    for m in range(half, n_ep):
        pass_relay(m)
        ready(m)
        expand(m)
        if m == half:
            contract(half - 1)
        if m - 2 >= half:
            pass_hidden(m - 2)
            contract(m - 2)
    pass_hidden(n_ep - 2)
    contract(n_ep - 2)
    pass_hidden(n_ep - 1)
    contract(n_ep - 1)

    total = None
    for m in range(n_ep):
        if m:
            back[m].wait_recv()
        high = matmul(whi[:, m * cap : (m + 1) * cap], ret[m])
        low = matmul(wlo[:, m * cap : (m + 1) * cap], ret[m])
        total = high + low if total is None else total + (high + low)
    o_ref[...] = total.astype(BF16)

    for copy in (send_halo, mix_partner, mix_across, mix_relay):
        copy.wait_send()
    for m in range(n_ep):
        for copy in (hid_partner[m], hid_across[m], hid_relay[m], from_source[m], back[m]):
            if copy is not None:
                copy.wait_send()
        for table in (to_partner, to_across, relay):
            if m in table:
                table[m].wait_send()


def fused(
    mixer_input,
    mixer_gain,
    outer_weight,
    inner_weight,
    value_weight,
    conv_kernel,
    group_gain,
    mixer_out_weight,
    expert_input,
    expert_gain,
    routes,
    route_weight,
    expert_gate,
    expert_up,
    expert_down,
):
    n_ep, n_tp = lax.axis_size("ep"), lax.axis_size("tp")
    rows, width = expert_input.shape
    mix_rows = mixer_input.shape[0]
    channels = outer_weight.shape[1]
    cap = 2 * routes.shape[1] * rows // n_ep
    span = width // n_tp
    part = expert_gate.shape[2]
    tile = 128
    tiles = part // tile
    full, out_cols = expert_down.shape[1:]
    mix_cols = mixer_out_weight.shape[1]
    vmem = pl.BlockSpec(memory_space=pltpu.VMEM)
    hbm = pl.BlockSpec(memory_space=pl.ANY)
    return pl.pallas_call(
        functools.partial(experts_kernel, n_ep),
        out_shape=(
            jax.ShapeDtypeStruct((mix_rows, mix_cols), BF16),
            jax.ShapeDtypeStruct((rows, out_cols), BF16),
        ),
        in_specs=[vmem] * 8 + [hbm] * 7,
        out_specs=(vmem, vmem),
        scratch_shapes=[
            pltpu.VMEM((rows, width), BF16),
            pltpu.VMEM((n_ep, 2, cap, span), BF16),
            pltpu.VMEM((n_ep, n_tp, cap, span), BF16),
            pltpu.VMEM((tiles, width, 2 * tile), BF16),
            pltpu.VMEM((full, out_cols), BF16),
            pltpu.VMEM((n_ep, n_tp, cap, part), BF16),
            pltpu.VMEM((n_ep, cap, out_cols), BF16),
            pltpu.VMEM((n_ep, cap, out_cols), BF16),
            pltpu.VMEM((rows, n_ep * cap), BF16),
            pltpu.VMEM((rows, n_ep * cap), BF16),
            pltpu.VMEM((mix_rows, width), BF16),
            pltpu.VMEM((3, width, channels), BF16),
            pltpu.VMEM((channels * n_tp, mix_cols), BF16),
            pltpu.VMEM((8 + mix_rows, channels), F32),
            pltpu.VMEM((mix_rows, channels), BF16),
            pltpu.VMEM((n_tp, mix_rows, channels), BF16),
            pltpu.SemaphoreType.DMA((2 * tiles + 5,)),
            pltpu.SemaphoreType.DMA((9, n_ep)),
            pltpu.SemaphoreType.DMA((9, n_ep)),
        ],
        compiler_params=pltpu.CompilerParams(
            collective_id=0, has_side_effects=True, vmem_limit_bytes=60 * 1024 * 1024
        ),
        name="layer",
    )(
        mixer_input,
        mixer_gain.reshape(1, -1),
        conv_kernel,
        group_gain.reshape(1, -1),
        expert_input,
        expert_gain.reshape(1, -1),
        routes.T,
        route_weight.T,
        outer_weight,
        inner_weight,
        value_weight,
        mixer_out_weight,
        expert_gate,
        expert_up,
        expert_down,
    )


def fits(n_ep, n_tp, routes, expert_gate):
    return (
        n_tp == 4
        and n_ep >= 4
        and n_ep & (n_ep - 1) == 0
        and routes.shape[1] == 2
        and expert_gate.shape[0] == 1
        and expert_gate.shape[2] % 128 == 0
    )


def mixer_xla(
    mixer_input,
    mixer_gain,
    outer_weight,
    inner_weight,
    value_weight,
    conv_kernel,
    group_gain,
    mixer_out_weight,
):
    mix_count = mixer_input.shape[0]
    normed_a = rms_scale(mixer_input, mixer_gain).astype(jnp.bfloat16)
    outer = jnp.dot(normed_a, outer_weight, preferred_element_type=jnp.float32).astype(jnp.bfloat16)
    inner = jnp.dot(normed_a, inner_weight, preferred_element_type=jnp.float32).astype(jnp.bfloat16)
    values = jnp.dot(normed_a, value_weight, preferred_element_type=jnp.float32).astype(
        jnp.bfloat16
    )
    product = inner.astype(jnp.float32) * values.astype(jnp.float32)
    earlier_rows = from_behind(product[mix_count - 2 :], "ep", 1)
    padded = jnp.concatenate([earlier_rows, product], axis=0)
    kernel = conv_kernel.astype(jnp.float32)
    conv_sum = (
        kernel[0] * padded[0:mix_count]
        + kernel[1] * padded[1 : mix_count + 1]
        + kernel[2] * padded[2 : mix_count + 2]
    )
    gated = outer.astype(jnp.float32) * conv_sum
    grouped = gated.reshape(mix_count, -1, GROUP)
    grouped = rms_scale(grouped, group_gain.reshape(-1, GROUP))
    grouped = grouped.reshape(mix_count, -1).astype(jnp.bfloat16)
    weight_rows = mixer_out_weight
    mixed_tokens = jnp.dot(
        lax.all_gather(grouped, "tp", axis=1, tiled=True),
        weight_rows,
        preferred_element_type=jnp.float32,
    ).astype(jnp.bfloat16)
    return mixed_tokens


def experts_xla(
    expert_input,
    expert_gain,
    routes,
    route_weight,
    expert_gate,
    expert_up,
    expert_down,
):
    exp_count, picks_each = routes.shape
    width = expert_input.shape[1]
    experts = expert_gate.shape[0] * lax.axis_size("ep")
    capacity = 2 * picks_each * exp_count // experts
    normed_b = rms_scale(expert_input, expert_gain).astype(jnp.bfloat16)
    picks = routes.reshape(-1)
    onehot = (picks[:, None] == jnp.arange(experts, dtype=jnp.int32)[None, :]).astype(jnp.int32)
    rank = jnp.sum((jnp.cumsum(onehot, axis=0) - onehot) * onehot, axis=1)
    slot = picks * capacity + rank
    token = jnp.arange(exp_count * picks_each, dtype=jnp.int32) // picks_each
    table = jnp.zeros((experts * capacity,), jnp.int32).at[slot].set(token + 1)
    valid = table > 0
    gathered_rows = jnp.take(normed_b, jnp.maximum(table - 1, 0), axis=0)
    buffer = jnp.where(valid[:, None], gathered_rows, 0).reshape(experts, capacity, width)
    gate_weight = expert_gate[0]
    up_weight = expert_up[0]
    down_weight = expert_down[0]
    out_cols = down_weight.shape[1]
    span = width // lax.axis_size("tp")
    outgoing = lax.dynamic_slice_in_dim(buffer, lax.axis_index("tp") * span, span, 2)
    received = lax.all_to_all(outgoing, "ep", split_axis=0, concat_axis=0, tiled=True)
    sources = received.shape[0]
    count = received.shape[1]
    piece = lax.all_gather(received, "tp", axis=2, tiled=True)
    span = piece.shape[2]
    flat_piece = piece.reshape(sources * count, span)
    gate = jnp.dot(flat_piece, gate_weight, preferred_element_type=jnp.float32)
    up_value = jnp.dot(flat_piece, up_weight, preferred_element_type=jnp.float32)
    hidden = (jax.nn.silu(gate) * up_value).astype(jnp.bfloat16)
    weight_rows = down_weight
    results = jnp.dot(
        lax.all_gather(hidden, "tp", axis=1, tiled=True),
        weight_rows,
        preferred_element_type=jnp.float32,
    ).astype(jnp.bfloat16)
    returned = lax.all_to_all(
        results.reshape(sources, count, out_cols), "ep", split_axis=0, concat_axis=0, tiled=True
    )
    flat_returned = returned.reshape(experts * capacity, out_cols)
    chosen = (
        jnp.take(flat_returned, slot, axis=0)
        .astype(jnp.float32)
        .reshape(exp_count, picks_each, out_cols)
    )
    weighted = jnp.sum(chosen * route_weight[..., None], axis=1)
    expert_tokens = weighted.astype(jnp.bfloat16)
    return expert_tokens


def per_device(*args):
    n_ep, n_tp = lax.axis_size("ep"), lax.axis_size("tp")
    if fits(n_ep, n_tp, args[10], args[12]):
        return fused(*args)
    return mixer_xla(*args[:8]), experts_xla(*args[8:])


def solution(mesh):
    placed = (
        P("ep", None),
        P(),
        P(None, "tp"),
        P(None, "tp"),
        P(None, "tp"),
        P(None, "tp"),
        P("tp"),
        P(None, "tp"),
        P("ep", None),
        P(),
        P("ep", None),
        P("ep", None),
        P("ep", None, "tp"),
        P("ep", None, "tp"),
        P("ep", None, "tp"),
    )
    return jax.shard_map(
        per_device,
        mesh=mesh,
        in_specs=placed,
        out_specs=(P("ep", "tp"), P("ep", "tp")),
        check_vma=False,
    )
```

```python
import functools

import jax
import jax.numpy as jnp
from jax import lax
from jax.experimental import pallas as pl
from jax.experimental.pallas import tpu as pltpu
from jax.sharding import PartitionSpec as P

GROUP = 64


EPS = 1e-06


def from_behind(block, axis, distance):
    devices = range(lax.axis_size(axis))
    route = [(i - distance, i) for i in devices if i - distance in devices]
    return lax.ppermute(block, axis, route)


def rms_scale(values, gain):
    floats = values.astype(jnp.float32)
    scale = lax.rsqrt(jnp.mean(floats * floats, axis=-1, keepdims=True) + EPS)
    return floats * scale * gain


F32 = jnp.float32
BF16 = jnp.bfloat16


def flip(index, offset, count):
    out = index
    bit = 1
    while bit < count:
        if offset & bit:
            out = out + bit - 2 * bit * ((index // bit) % 2)
        bit *= 2
    return out


def matmul(a, b):
    return jnp.dot(a, b, preferred_element_type=F32)


def send_order(n_ep):
    half = n_ep // 2
    return [1, *range(half, n_ep), *range(2, half)]


def schedule(n_ep):
    half = n_ep // 2
    early = [*range(half, half + half // 2)]
    late = [*range(half + half // 2, n_ep)]
    steps = [("pass_far", m) for m in early]
    steps += [("finish", 0), ("mix", 0)]
    steps += [("far", m) for m in early] + [("pass_far", m) for m in late] + [("finish", 1)]
    done = list(early)
    for m, other in zip(range(2, half), late):
        steps += [("near", m), ("finish", done.pop(0)), ("far", other), ("finish", done.pop(0))]
        done += [m, other]
    return steps + [("finish", m) for m in done]


def experts_kernel(
    n_ep,
    mix_ref,
    mix_gain_ref,
    kernel_ref,
    group_gain_ref,
    x_ref,
    gain_ref,
    routes_ref,
    weight_ref,
    outer_hbm,
    inner_hbm,
    value_hbm,
    mix_out_hbm,
    gate_hbm,
    up_hbm,
    down_hbm,
    mix_o_ref,
    o_ref,
    nb,
    xs,
    xb,
    wgu,
    wd,
    hb,
    rs,
    ret,
    whi,
    wlo,
    na,
    wmix,
    wmo,
    padded,
    outer,
    grouped,
    w_sem,
    s_sem,
    r_sem,
):
    ep = lax.axis_index("ep")
    tp = lax.axis_index("tp")
    y, core = tp // 2, tp % 2
    partner = {"tp": y * 2 + 1 - core}
    across = {"tp": (1 - y) * 2 + core}
    over_tp = (1 - y) * 2 + core
    half = n_ep // 2
    rows = x_ref.shape[0]
    cap = xb.shape[2]
    span = xb.shape[3]
    tiles, depth, pair = wgu.shape
    tile = pair // 2
    part = hb.shape[3]
    out_cols = wd.shape[1]

    barrier = pltpu.get_barrier_semaphore()
    peers = [{"ep": flip(ep, m, n_ep)} for m in range(1, n_ep)] + [partner, across]
    for peer in peers:
        pl.semaphore_signal(barrier, inc=1, device_id=peer, device_id_type=pl.DeviceIdType.MESH)

    fetches = []
    for j in range(tiles):
        cols = pl.ds(j * tile, tile)
        fetches.append(
            (
                pltpu.make_async_copy(
                    gate_hbm.at[0, :, cols], wgu.at[j, :, pl.ds(0, tile)], w_sem.at[2 * j]
                ),
                pltpu.make_async_copy(
                    up_hbm.at[0, :, cols], wgu.at[j, :, pl.ds(tile, tile)], w_sem.at[2 * j + 1]
                ),
            )
        )
    fetch_down = pltpu.make_async_copy(down_hbm.at[0], wd, w_sem.at[2 * tiles])
    fetch_mix = [
        pltpu.make_async_copy(src, wmix.at[i], w_sem.at[2 * tiles + 1 + i])
        for i, src in enumerate((outer_hbm, inner_hbm, value_hbm))
    ]
    fetch_mix_out = pltpu.make_async_copy(mix_out_hbm, wmo, w_sem.at[2 * tiles + 4])
    for a, b in fetches:
        a.start()
        b.start()
    for copy in fetch_mix:
        copy.start()
    fetch_down.start()
    fetch_mix_out.start()

    step_rows = 32

    def normalize(src, gain, dst):
        def norm(i, carry):
            at = pl.ds(pl.multiple_of(i * step_rows, step_rows), step_rows)
            v = src[at, :].astype(F32)
            scale = lax.rsqrt(jnp.mean(v * v, axis=-1, keepdims=True) + EPS)
            dst[at, :] = (v * scale * gain[...]).astype(BF16)
            return carry

        lax.fori_loop(0, src.shape[0] // step_rows, norm, 0)

    normalize(x_ref, gain_ref, nb)

    first = routes_ref[0:1, :]
    second = routes_ref[1:2, :]
    masks = []
    level = lax.broadcasted_iota(jnp.int32, (n_ep, rows), 0)
    stacked = jnp.zeros((n_ep, rows), F32)
    for m in range(n_ep):
        e = flip(ep, m, n_ep)
        mask = jnp.where((first == e) | (second == e), 1.0, 0.0)
        masks.append(mask)
        stacked = jnp.where(level == m, mask, stacked)
    upper = lax.broadcasted_iota(jnp.int32, (rows, rows), 0) < lax.broadcasted_iota(
        jnp.int32, (rows, rows), 1
    )
    ranks = matmul(stacked.astype(BF16), jnp.where(upper, 1.0, 0.0).astype(BF16))
    slots = lax.broadcasted_iota(jnp.int32, (cap, rows), 0).astype(F32)
    place = []
    for m in range(n_ep):
        place.append(jnp.where((slots == ranks[m : m + 1, :]) & (masks[m] > 0.5), 1.0, 0.0))

    def remote(src, dst, kind, m, device):
        return pltpu.make_async_remote_copy(
            src_ref=src,
            dst_ref=dst,
            send_sem=s_sem.at[kind, m],
            recv_sem=r_sem.at[kind, m],
            device_id=device,
            device_id_type=pl.DeviceIdType.MESH,
        )

    mine2 = pl.ds(core * 2, 2)
    from_source, to_partner, to_across, relay = [None] * n_ep, {}, {}, {}
    for m in range(1, n_ep):
        peer = {"ep": flip(ep, m, n_ep)}
        if m < half:
            from_source[m] = remote(xs.at[m], xb.at[m, mine2], 0, m, peer)
            to_partner[m] = remote(xb.at[m, mine2], xb.at[m, mine2], 1, m, partner)
        else:
            from_source[m] = remote(xs.at[m, 0], xb.at[m, tp], 0, m, peer)
            to_partner[m] = remote(xb.at[m, tp], xb.at[m, tp], 1, m, partner)
            to_across[m] = remote(xb.at[m, tp], xb.at[m, tp], 2, m, across)
            relay[m] = remote(xb.at[m, over_tp], xb.at[m, over_tp], 3, m, partner)
    hid_partner, hid_across, hid_relay, back = [], [], [], [None] * n_ep
    for m in range(n_ep):
        hid_partner.append(remote(hb.at[m, tp], hb.at[m, tp], 4, m, partner))
        hid_across.append(remote(hb.at[m, tp], hb.at[m, tp], 5, m, across))
        hid_relay.append(remote(hb.at[m, over_tp], hb.at[m, over_tp], 6, m, partner))
        if m:
            back[m] = remote(rs.at[m], ret.at[m], 7, m, {"ep": flip(ep, m, n_ep)})

    for m in send_order(n_ep):
        chosen = place[m].astype(BF16)
        if m < half:
            for k in range(2):
                at = pl.ds(pl.multiple_of((core * 2 + k) * span, span), span)
                xs[m, k] = matmul(chosen, nb[:, at]).astype(BF16)
        else:
            at = pl.ds(pl.multiple_of(tp * span, span), span)
            xs[m, 0] = matmul(chosen, nb[:, at]).astype(BF16)
        if m == send_order(n_ep)[0]:
            pl.semaphore_wait(barrier, len(peers))
        from_source[m].start()
    chosen = place[0].astype(BF16)
    for k in range(depth // span):
        xb[0, k] = matmul(chosen, nb[:, k * span : (k + 1) * span]).astype(BF16)

    def expand(m):
        def body(j, carry):
            if m == 0:
                pltpu.make_async_copy(
                    gate_hbm.at[0, :, pl.ds(0, tile)], wgu.at[j, :, pl.ds(0, tile)], w_sem.at[2 * j]
                ).wait()
                pltpu.make_async_copy(
                    up_hbm.at[0, :, pl.ds(0, tile)],
                    wgu.at[j, :, pl.ds(tile, tile)],
                    w_sem.at[2 * j + 1],
                ).wait()
            acc = matmul(xb[m, 0], wgu[j, 0:span, :])
            for k in range(1, depth // span):
                acc = acc + matmul(xb[m, k], wgu[j, k * span : (k + 1) * span, :])
            g, u = acc[:, :tile], acc[:, tile:]
            hidden = g / (1.0 + jnp.exp(-g)) * u
            hb[m, tp, :, pl.ds(pl.multiple_of(j * tile, tile), tile)] = hidden.astype(BF16)
            return carry

        lax.fori_loop(0, tiles, body, 0)
        hid_across[m].start()
        hid_partner[m].start()

    block = 256

    def contract(m):
        hid_partner[m].wait_recv()
        hid_relay[m].wait_recv()
        for n in range(out_cols // block):
            cols = slice(n * block, (n + 1) * block)
            acc = matmul(hb[m, 0], wd[0:part, cols])
            for k in range(1, hb.shape[1]):
                acc = acc + matmul(hb[m, k], wd[k * part : (k + 1) * part, cols])
            if m == 0:
                ret[0, :, cols] = acc.astype(BF16)
            else:
                rs[m, :, cols] = acc.astype(BF16)
        if m:
            back[m].start()

    def pass_hidden(m):
        hid_across[m].wait_recv()
        hid_relay[m].start()

    def pass_near(m):
        from_source[m].wait_recv()
        to_partner[m].start()

    def pass_far(m):
        from_source[m].wait_recv()
        to_across[m].start()
        to_partner[m].start()

    def pass_relay(m):
        to_across[m].wait_recv()
        relay[m].start()

    def ready(m):
        to_partner[m].wait_recv()
        if m >= half:
            relay[m].wait_recv()

    mix_rows, channels = outer.shape
    halo = padded.shape[0] - mix_rows
    ahead = {"ep": lax.rem(ep + 1, n_ep)}
    send_halo = remote(padded.at[pl.ds(mix_rows, halo)], padded.at[pl.ds(0, halo)], 8, 0, ahead)
    mix_partner = remote(grouped.at[tp], grouped.at[tp], 8, 1, partner)
    mix_across = remote(grouped.at[tp], grouped.at[tp], 8, 2, across)
    mix_relay = remote(grouped.at[over_tp], grouped.at[over_tp], 8, 3, partner)

    def mix_project():
        normalize(mix_ref, mix_gain_ref, na)
        for copy in fetch_mix:
            copy.wait()
        outer[...] = matmul(na[...], wmix[0]).astype(BF16)
        inner = matmul(na[...], wmix[1]).astype(BF16).astype(F32)
        padded[pl.ds(halo, mix_rows), :] = inner * matmul(na[...], wmix[2]).astype(BF16).astype(F32)
        send_halo.start()

    def mix_convolve():
        send_halo.wait_recv()
        taps = kernel_ref[...].astype(F32)
        row = lax.broadcasted_iota(jnp.int32, (mix_rows, channels), 0)
        row = row + jnp.where(ep == 0, 0, mix_rows)
        conv = taps[2:3, :] * padded[pl.ds(halo, mix_rows), :]
        for back_by in (1, 2):
            shifted = padded[pl.ds(halo - back_by, mix_rows), :]
            conv = conv + taps[2 - back_by : 3 - back_by, :] * jnp.where(
                row >= back_by, shifted, 0.0
            )
        gated = outer[...].astype(F32) * conv
        squares = gated * gated
        group = lax.broadcasted_iota(jnp.int32, (mix_rows, channels), 1) // GROUP
        scale = jnp.zeros_like(gated)
        for i in range(channels // GROUP):
            mean = jnp.sum(jnp.where(group == i, squares, 0.0), axis=-1, keepdims=True) / GROUP
            scale = jnp.where(group == i, lax.rsqrt(mean + EPS), scale)
        grouped[tp] = (gated * scale * group_gain_ref[...]).astype(BF16)
        mix_across.start()
        mix_partner.start()

    def mix_pass():
        mix_across.wait_recv()
        mix_relay.start()

    def mix_contract():
        fetch_mix_out.wait()
        mix_partner.wait_recv()
        mix_relay.wait_recv()
        acc = matmul(grouped[0], wmo[0:channels, :])
        for k in range(1, grouped.shape[0]):
            acc = acc + matmul(grouped[k], wmo[k * channels : (k + 1) * channels, :])
        mix_o_ref[...] = acc.astype(BF16)

    def build_weights():
        for m in range(n_ep):
            picked = jnp.where(first == flip(ep, m, n_ep), weight_ref[0:1, :], weight_ref[1:2, :])
            scaled = (place[m] * picked).T
            high = scaled.astype(BF16)
            whi[:, m * cap : (m + 1) * cap] = high
            wlo[:, m * cap : (m + 1) * cap] = (scaled - high.astype(F32)).astype(BF16)

    def near(m):
        pass_near(m)
        ready(m)
        expand(m)

    def far(m):
        pass_relay(m)
        ready(m)
        expand(m)

    def finish(m):
        pass_hidden(m)
        contract(m)

    steps = dict(
        near=near, far=far, finish=finish, pass_far=pass_far, pass_hidden=pass_hidden,
        contract=contract,
    )
    expand(0)
    mix_project()
    build_weights()
    near(1)
    mix_convolve()
    fetch_down.wait()
    for step, m in schedule(n_ep):
        if step == "mix":
            mix_pass()
            mix_contract()
        else:
            steps[step](m)

    total = None
    for m in range(n_ep):
        if m:
            back[m].wait_recv()
        high = matmul(whi[:, m * cap : (m + 1) * cap], ret[m])
        low = matmul(wlo[:, m * cap : (m + 1) * cap], ret[m])
        total = high + low if total is None else total + (high + low)
    o_ref[...] = total.astype(BF16)

    for copy in (send_halo, mix_partner, mix_across, mix_relay):
        copy.wait_send()
    for m in range(n_ep):
        for copy in (hid_partner[m], hid_across[m], hid_relay[m], from_source[m], back[m]):
            if copy is not None:
                copy.wait_send()
        for table in (to_partner, to_across, relay):
            if m in table:
                table[m].wait_send()


def fused(
    mixer_input,
    mixer_gain,
    outer_weight,
    inner_weight,
    value_weight,
    conv_kernel,
    group_gain,
    mixer_out_weight,
    expert_input,
    expert_gain,
    routes,
    route_weight,
    expert_gate,
    expert_up,
    expert_down,
):
    n_ep, n_tp = lax.axis_size("ep"), lax.axis_size("tp")
    rows, width = expert_input.shape
    mix_rows = mixer_input.shape[0]
    channels = outer_weight.shape[1]
    cap = 2 * routes.shape[1] * rows // n_ep
    span = width // n_tp
    part = expert_gate.shape[2]
    tile = 128
    tiles = part // tile
    full, out_cols = expert_down.shape[1:]
    mix_cols = mixer_out_weight.shape[1]
    vmem = pl.BlockSpec(memory_space=pltpu.VMEM)
    hbm = pl.BlockSpec(memory_space=pl.ANY)
    return pl.pallas_call(
        functools.partial(experts_kernel, n_ep),
        out_shape=(
            jax.ShapeDtypeStruct((mix_rows, mix_cols), BF16),
            jax.ShapeDtypeStruct((rows, out_cols), BF16),
        ),
        in_specs=[vmem] * 8 + [hbm] * 7,
        out_specs=(vmem, vmem),
        scratch_shapes=[
            pltpu.VMEM((rows, width), BF16),
            pltpu.VMEM((n_ep, 2, cap, span), BF16),
            pltpu.VMEM((n_ep, n_tp, cap, span), BF16),
            pltpu.VMEM((tiles, width, 2 * tile), BF16),
            pltpu.VMEM((full, out_cols), BF16),
            pltpu.VMEM((n_ep, n_tp, cap, part), BF16),
            pltpu.VMEM((n_ep, cap, out_cols), BF16),
            pltpu.VMEM((n_ep, cap, out_cols), BF16),
            pltpu.VMEM((rows, n_ep * cap), BF16),
            pltpu.VMEM((rows, n_ep * cap), BF16),
            pltpu.VMEM((mix_rows, width), BF16),
            pltpu.VMEM((3, width, channels), BF16),
            pltpu.VMEM((channels * n_tp, mix_cols), BF16),
            pltpu.VMEM((8 + mix_rows, channels), F32),
            pltpu.VMEM((mix_rows, channels), BF16),
            pltpu.VMEM((n_tp, mix_rows, channels), BF16),
            pltpu.SemaphoreType.DMA((2 * tiles + 5,)),
            pltpu.SemaphoreType.DMA((9, n_ep)),
            pltpu.SemaphoreType.DMA((9, n_ep)),
        ],
        compiler_params=pltpu.CompilerParams(
            collective_id=0, has_side_effects=True, vmem_limit_bytes=60 * 1024 * 1024
        ),
        name="layer",
    )(
        mixer_input,
        mixer_gain.reshape(1, -1),
        conv_kernel,
        group_gain.reshape(1, -1),
        expert_input,
        expert_gain.reshape(1, -1),
        routes.T,
        route_weight.T,
        outer_weight,
        inner_weight,
        value_weight,
        mixer_out_weight,
        expert_gate,
        expert_up,
        expert_down,
    )


def fits(n_ep, n_tp, routes, expert_gate):
    return (
        n_tp == 4
        and n_ep >= 4
        and n_ep & (n_ep - 1) == 0
        and routes.shape[1] == 2
        and expert_gate.shape[0] == 1
        and expert_gate.shape[2] % 128 == 0
    )


def mixer_xla(
    mixer_input,
    mixer_gain,
    outer_weight,
    inner_weight,
    value_weight,
    conv_kernel,
    group_gain,
    mixer_out_weight,
):
    mix_count = mixer_input.shape[0]
    normed_a = rms_scale(mixer_input, mixer_gain).astype(jnp.bfloat16)
    outer = jnp.dot(normed_a, outer_weight, preferred_element_type=jnp.float32).astype(jnp.bfloat16)
    inner = jnp.dot(normed_a, inner_weight, preferred_element_type=jnp.float32).astype(jnp.bfloat16)
    values = jnp.dot(normed_a, value_weight, preferred_element_type=jnp.float32).astype(
        jnp.bfloat16
    )
    product = inner.astype(jnp.float32) * values.astype(jnp.float32)
    earlier_rows = from_behind(product[mix_count - 2 :], "ep", 1)
    padded = jnp.concatenate([earlier_rows, product], axis=0)
    kernel = conv_kernel.astype(jnp.float32)
    conv_sum = (
        kernel[0] * padded[0:mix_count]
        + kernel[1] * padded[1 : mix_count + 1]
        + kernel[2] * padded[2 : mix_count + 2]
    )
    gated = outer.astype(jnp.float32) * conv_sum
    grouped = gated.reshape(mix_count, -1, GROUP)
    grouped = rms_scale(grouped, group_gain.reshape(-1, GROUP))
    grouped = grouped.reshape(mix_count, -1).astype(jnp.bfloat16)
    weight_rows = mixer_out_weight
    mixed_tokens = jnp.dot(
        lax.all_gather(grouped, "tp", axis=1, tiled=True),
        weight_rows,
        preferred_element_type=jnp.float32,
    ).astype(jnp.bfloat16)
    return mixed_tokens


def experts_xla(
    expert_input,
    expert_gain,
    routes,
    route_weight,
    expert_gate,
    expert_up,
    expert_down,
):
    exp_count, picks_each = routes.shape
    width = expert_input.shape[1]
    experts = expert_gate.shape[0] * lax.axis_size("ep")
    capacity = 2 * picks_each * exp_count // experts
    normed_b = rms_scale(expert_input, expert_gain).astype(jnp.bfloat16)
    picks = routes.reshape(-1)
    onehot = (picks[:, None] == jnp.arange(experts, dtype=jnp.int32)[None, :]).astype(jnp.int32)
    rank = jnp.sum((jnp.cumsum(onehot, axis=0) - onehot) * onehot, axis=1)
    slot = picks * capacity + rank
    token = jnp.arange(exp_count * picks_each, dtype=jnp.int32) // picks_each
    table = jnp.zeros((experts * capacity,), jnp.int32).at[slot].set(token + 1)
    valid = table > 0
    gathered_rows = jnp.take(normed_b, jnp.maximum(table - 1, 0), axis=0)
    buffer = jnp.where(valid[:, None], gathered_rows, 0).reshape(experts, capacity, width)
    gate_weight = expert_gate[0]
    up_weight = expert_up[0]
    down_weight = expert_down[0]
    out_cols = down_weight.shape[1]
    span = width // lax.axis_size("tp")
    outgoing = lax.dynamic_slice_in_dim(buffer, lax.axis_index("tp") * span, span, 2)
    received = lax.all_to_all(outgoing, "ep", split_axis=0, concat_axis=0, tiled=True)
    sources = received.shape[0]
    count = received.shape[1]
    piece = lax.all_gather(received, "tp", axis=2, tiled=True)
    span = piece.shape[2]
    flat_piece = piece.reshape(sources * count, span)
    gate = jnp.dot(flat_piece, gate_weight, preferred_element_type=jnp.float32)
    up_value = jnp.dot(flat_piece, up_weight, preferred_element_type=jnp.float32)
    hidden = (jax.nn.silu(gate) * up_value).astype(jnp.bfloat16)
    weight_rows = down_weight
    results = jnp.dot(
        lax.all_gather(hidden, "tp", axis=1, tiled=True),
        weight_rows,
        preferred_element_type=jnp.float32,
    ).astype(jnp.bfloat16)
    returned = lax.all_to_all(
        results.reshape(sources, count, out_cols), "ep", split_axis=0, concat_axis=0, tiled=True
    )
    flat_returned = returned.reshape(experts * capacity, out_cols)
    chosen = (
        jnp.take(flat_returned, slot, axis=0)
        .astype(jnp.float32)
        .reshape(exp_count, picks_each, out_cols)
    )
    weighted = jnp.sum(chosen * route_weight[..., None], axis=1)
    expert_tokens = weighted.astype(jnp.bfloat16)
    return expert_tokens


def per_device(*args):
    n_ep, n_tp = lax.axis_size("ep"), lax.axis_size("tp")
    if fits(n_ep, n_tp, args[10], args[12]):
        return fused(*args)
    return mixer_xla(*args[:8]), experts_xla(*args[8:])


def solution(mesh):
    placed = (
        P("ep", None),
        P(),
        P(None, "tp"),
        P(None, "tp"),
        P(None, "tp"),
        P(None, "tp"),
        P("tp"),
        P(None, "tp"),
        P("ep", None),
        P(),
        P("ep", None),
        P("ep", None),
        P("ep", None, "tp"),
        P("ep", None, "tp"),
        P("ep", None, "tp"),
    )
    return jax.shard_map(
        per_device,
        mesh=mesh,
        in_specs=placed,
        out_specs=(P("ep", "tp"), P("ep", "tp")),
        check_vma=False,
    )
```
